32 devices in a mesh: grp: 2 (over y), ep: 8 (over z, core), tp: 2 (over x).
Axes of the slice: x: 2, y: 2, z: 4, core: 2. Of those that a mesh axis runs over, the one named last changes fastest.
Arguments:
- recurrence_query_input: bfloat16 [2048, 2048], P(('grp', 'ep'), 'tp'), parts along dimension 0, may hold values from -6 to 6
- forget_gate_input: bfloat16 [2048, 2048], P(('grp', 'ep'), 'tp'), parts along dimension 0, may hold values from -6.5 to 6.5
- recurrence_value_input: bfloat16 [2048, 2048], P(('grp', 'ep'), 'tp'), parts along dimension 0, may hold values from -6 to 6
- output_gate_input: bfloat16 [2048, 2048], P(('grp', 'ep'), 'tp'), parts along dimension 0, may hold values from -6 to 6
- forget_lower_margin: float32 [2048], P('tp'), may hold values from 0 to 0.1
- position_decay_extra: float32 [2048, 16], P(('grp', 'ep'), 'tp'), parts along dimension 0, may hold values from -2.1 to 0
- head_norm_gain: float32 [2048], P('tp'), may hold values from 0.1 to 1.9
- recurrence_out_weight: bfloat16 [2048, 2048], P('tp'), may hold values from -0.125 to 0.125
- expert_hidden_state: bfloat16 [2048, 2048], P(('grp', 'ep')), parts along dimension 0, may hold values from -6 to 6
- chosen_expert_index: int32 [2048, 4], P(('grp', 'ep')), parts along dimension 0, may hold values from 0 to 7, all different within a row; in each aligned block of 128 rows (0 to 127, 128 to 255, ...) at most 128 rows name the same one
- chosen_expert_score: float32 [2048, 4], P(('grp', 'ep')), parts along dimension 0, may hold values from 0.02 to 1
- expert_norm_gain: float32 [2048], replicated, may hold values from 0.1 to 1.9
- routed_gate_weight: bfloat16 [8, 2048, 1024], P('ep', None, 'tp'), may hold values from -0.125 to 0.125
- routed_up_weight: bfloat16 [8, 2048, 1024], P('ep', None, 'tp'), may hold values from -0.125 to 0.125
- routed_down_weight: bfloat16 [8, 1024, 2048], P('ep', None, 'tp'), may hold values from -0.1875 to 0.1875
- shared_gate_weight: bfloat16 [2048, 1024], P(None, 'tp'), may hold values from -0.125 to 0.125
- shared_up_weight: bfloat16 [2048, 1024], P(None, 'tp'), may hold values from -0.125 to 0.125
- shared_down_weight: bfloat16 [1024, 2048], P(None, 'tp'), may hold values from -0.1875 to 0.1875
Outputs:
- recurrence_output: bfloat16 [2048, 2048], P(('grp', 'ep', 'tp')), parts along dimension 0
- expert_out: bfloat16 [2048, 2048], P(('grp', 'ep'), 'tp'), parts along dimension 0
The draws below stay inside these ranges and needn't reach their ends.
There are 2 independent parts, one for each index of `grp`. The reference program is written for one: setup_inputs(seed, part) draws one part's arguments, and reference() takes and returns one part's arrays. A program takes and returns all parts, laid end to end along the dimension named above; an argument that names none is the same for every part. Nothing has to cross between parts.
Inputs may be any that keep to these rules, and one draw needn't show every extreme that they name: `chosen_expert_index`: each row names 4 different experts. In each aligned block of 128 rows (the rows of one index of ep) no expert is named by more than 128 rows, and in every draw some block names some expert exactly 128 times.
All inputs are finite; a program needn't handle non-finite values.
Results may differ from the reference program's by a relative error of at most 0.015.
Values may be sent and summed in bfloat16 or wider, within the bound.
A program may use at most 64 MiB of HBM per device.

```python
import math
import jax
import jax.numpy as jnp
import numpy as np
from jax import lax

D = 2048
HEADS = 16
HEAD_CHANNELS = 128
W = 2048
BLK = 64
FF = 1024
TOP_K = 4
EXPERTS = 8
TOKA_DEV = 128
TOKB_DEV = 128
SEQ_A = 1024
TOK_B = 1024
CAP = 128
N_EP = 8
N_TP = 2


def draw_forget_gate_input(key, part):
    noise_key, shift_key = jax.random.split(jax.random.fold_in(key, 11))
    noise = jnp.clip(jax.random.normal(noise_key, (SEQ_A, W), jnp.float32), -5.0, 5.0)
    shifts = jax.random.uniform(shift_key, (SEQ_A // TOKA_DEV, 1, 1), jnp.float32, -1.5, 1.5)
    shifted = noise.reshape(SEQ_A // TOKA_DEV, TOKA_DEV, W) + shifts
    return shifted.reshape(SEQ_A, W).astype(jnp.bfloat16)


def draw_forget_lower_margin(key, part):
    pick_key, slow_key, fast_key = jax.random.split(jax.random.fold_in(key, 23), 3)
    slow_count = HEADS // 2
    slow_heads = (jax.random.permutation(pick_key, HEADS) < slow_count)[:, None]
    slow = 2.0 * jnp.exp(jax.random.uniform(slow_key, (HEADS, HEAD_CHANNELS), jnp.float32, math.log(0.1), math.log(0.6))) / SEQ_A
    fast = jnp.exp(jax.random.uniform(fast_key, (HEADS, HEAD_CHANNELS), jnp.float32, math.log(0.03), math.log(0.09)))
    return jnp.where(slow_heads, slow, fast).reshape(W).astype(jnp.float32)


def draw_position_decay_extra(key, part):
    place_key, depth_key, count_key = jax.random.split(jax.random.fold_in(key, 37), 3)
    spots = jax.random.randint(place_key, (3, HEADS), 0, SEQ_A)
    counts = jax.random.randint(count_key, (1, HEADS), 1, 4)
    active = jnp.arange(3)[:, None] < counts
    depth = jnp.log(jax.random.uniform(depth_key, (3, HEADS), jnp.float32, 0.5, 0.8))
    positions = jnp.arange(SEQ_A)[:, None, None]
    hits = (positions == spots[None]) & active[None]
    return jnp.sum(jnp.where(hits, depth[None], 0.0), axis=1).astype(jnp.float32)


def levels(rng, shape, pieces, smallest, largest):
    def one(axis_at, parts):
        heights = jax.random.uniform(jax.random.fold_in(jax.random.fold_in(rng, 6), axis_at), (parts,), jnp.float32, smallest / len(pieces), largest / len(pieces))
        return jnp.repeat(jnp.exp(heights), shape[axis_at] // parts).reshape((-1,) + (1,) * (len(shape) - axis_at - 1))

    factor_of = one(*pieces[0])
    for cut in pieces[1:]:
        factor_of = factor_of * one(*cut)
    return factor_of


def shared_out(key, own, number, rows, number_of, top, reach, skew):
    sequence = jax.random.permutation(key, number_of)
    packed, common = load_shares(number_of, rows * top, reach, skew, True), load_shares(number_of, rows * top, reach, skew, False)
    places = jnp.arange(number_of)

    def named(tallies, turn):
        used = int((tallies > 0).sum())
        fixed = max(1, used // 4)
        moved = fixed + (places - fixed + turn * (used - fixed)) % max(1, number_of - fixed)
        return jnp.zeros((number_of,), jnp.int32).at[sequence[jnp.where(places < fixed, places, moved)]].set(jnp.asarray(tallies, jnp.int32))

    tallies = jnp.where(number % 4 == 0, named(packed, number // 4), named(common, number - number // 4 - 1))
    mixed = jax.random.permutation(jax.random.fold_in(own, 3), number_of)
    giver, taker = mixed[0:number_of // 2 * 2:2], mixed[1:number_of // 2 * 2:2]
    margin = jnp.minimum(tallies[giver] - 1, reach - tallies[taker]) // 2
    margin = jnp.where((giver == sequence[0]) | (taker == sequence[0]) | (tallies[taker] == 0), 0, jnp.maximum(margin, 0))
    moved = jax.random.randint(jax.random.fold_in(own, 4), (number_of // 2,), 0, 1 << 20) % (margin + 1)
    tallies = tallies.at[giver].add(-moved).at[taker].add(moved)
    members = jnp.searchsorted(jnp.cumsum(tallies), jnp.arange(rows * top), side="right").astype(jnp.int32)
    table = members.reshape(top, rows).T
    table = table[jax.random.permutation(jax.random.fold_in(own, 1), rows)]
    turn = jax.random.randint(jax.random.fold_in(own, 2), (rows, 1), 0, top)
    return jnp.take_along_axis(table, (jnp.arange(top)[None, :] + turn) % top, axis=1)


def load_shares(count, total, limit, lean, full):
    portions = [(1 << 20) // math.isqrt(standing ** lean) + 1 for standing in range(1, count + 1)]
    largest = limit if full else min(limit, max(-(-total // count), total * portions[0] // sum(portions)))
    least = 1 if total - largest >= count - 1 else 0
    holding, spare = [largest] + [least] * (count - 1), total - largest - least * (count - 1)
    while spare > 0:
        free = [i for i in range(1, count) if holding[i] < largest] or [i for i in range(1, count) if holding[i] < limit]
        pool, remaining = sum([portions[i] for i in free]), spare
        for i in free:
            more = min(limit - holding[i], max(1, remaining * portions[i] // pool), spare)
            holding[i] = holding[i] + more
            spare = spare - more
    return np.array(holding)


def gaussian(key, extent, width, reach, cuts=(), held_as=jnp.bfloat16):
    entries = jax.random.normal(key, extent, jnp.float32) * width
    if len(cuts) > 0:
        entries = levels(key, extent, cuts, -0.22, 0.18) * entries
    return jnp.clip(entries, min=-reach, max=reach).astype(held_as)


def setup_inputs(seed: int = 0, part: int = 0) -> dict:
    keys = jax.random.split(jax.random.key(seed), 19)
    part_splits = jax.random.split(jax.random.fold_in(keys[18], part), 19)
    recurrence_query_input = gaussian(part_splits[0], (SEQ_A, W), 1.0, 6.0, ((0, 8), (1, 2)))
    forget_gate_input = draw_forget_gate_input(jax.random.fold_in(jax.random.fold_in(keys[18], part), 71), part)
    recurrence_value_input = gaussian(part_splits[2], (SEQ_A, W), 1.0, 6.0, ((0, 8), (1, 2)))
    output_gate_input = gaussian(part_splits[3], (SEQ_A, W), 1.0, 6.0, ((0, 8), (1, 2)))
    forget_lower_margin = draw_forget_lower_margin(jax.random.fold_in(keys[18], 71), part)
    position_decay_extra = draw_position_decay_extra(jax.random.fold_in(jax.random.fold_in(keys[18], part), 71), part)
    head_norm_gain = jnp.clip(1.0 + 0.18 * jax.random.normal(keys[6], (W,), jnp.float32), 0.1, 1.9)
    recurrence_out_weight = gaussian(keys[7], (W, D), W ** -0.5, 0.125, ((0, 2),))
    expert_hidden_state = gaussian(part_splits[8], (TOK_B, D), 1.0, 6.0, ((0, 8),))
    chosen_expert_index_keys = jax.random.split(jax.random.fold_in(part_splits[9], 1), TOK_B // TOKB_DEV)
    chosen_expert_index_turns = jax.random.permutation(jax.random.fold_in(part_splits[9], 3), TOK_B // TOKB_DEV)
    chosen_expert_index = jax.vmap(lambda own, number: shared_out(jax.random.fold_in(part_splits[9], 2), own, number, TOKB_DEV, EXPERTS, TOP_K, CAP, 1))(chosen_expert_index_keys, chosen_expert_index_turns).reshape((TOK_B, TOP_K))
    chosen_expert_score = jnp.clip(jnp.exp(math.log(1.0) - 3.912023 * jax.random.uniform(part_splits[10], (TOK_B, TOP_K), jnp.float32) ** levels(part_splits[10], (TOK_B, TOP_K), ((0, 8),), -0.2, 0.2)), 0.02, 1.0)
    expert_norm_gain = jnp.clip(1.0 + 0.18 * jax.random.normal(keys[11], (D,), jnp.float32), 0.1, 1.9)
    routed_gate_weight = gaussian(keys[12], (EXPERTS, D, FF), D ** -0.5, 0.125, ((0, 8), (2, 2)))
    routed_up_weight = gaussian(keys[13], (EXPERTS, D, FF), D ** -0.5, 0.125, ((0, 8), (2, 2)))
    routed_down_weight = gaussian(keys[14], (EXPERTS, FF, D), FF ** -0.5, 0.1875, ((0, 8), (2, 2)))
    shared_gate_weight = gaussian(keys[15], (D, FF), D ** -0.5, 0.125, ((1, 2),))
    shared_up_weight = gaussian(keys[16], (D, FF), D ** -0.5, 0.125, ((1, 2),))
    shared_down_weight = gaussian(keys[17], (FF, D), FF ** -0.5, 0.1875, ((1, 2),))
    return dict(recurrence_query_input=recurrence_query_input, forget_gate_input=forget_gate_input, recurrence_value_input=recurrence_value_input, output_gate_input=output_gate_input, forget_lower_margin=forget_lower_margin, position_decay_extra=position_decay_extra, head_norm_gain=head_norm_gain, recurrence_out_weight=recurrence_out_weight, expert_hidden_state=expert_hidden_state, chosen_expert_index=chosen_expert_index, chosen_expert_score=chosen_expert_score, expert_norm_gain=expert_norm_gain, routed_gate_weight=routed_gate_weight, routed_up_weight=routed_up_weight, routed_down_weight=routed_down_weight, shared_gate_weight=shared_gate_weight, shared_up_weight=shared_up_weight, shared_down_weight=shared_down_weight)


EPSILON = 1e-06
ROUTED_SCALE = 2.5
HIGHEST_PRECISION = lax.Precision.HIGHEST

def recurrence(queries, key_gate_value, decay_logarithm, value_rows):
    length = queries.shape[0]
    blocks = length // BLK

    def split_heads(tensor):
        return tensor.reshape(blocks, BLK, HEADS, HEAD_CHANNELS).transpose(2, 0, 1, 3)
    query_heads = split_heads(queries)
    key_heads = split_heads(key_gate_value)
    value_heads = split_heads(value_rows)
    cum_decay = jnp.cumsum(split_heads(decay_logarithm), axis=2)
    middle = cum_decay[:, :, BLK // 2 - 1:BLK // 2]
    block_end = cum_decay[:, :, BLK - 1:BLK]
    scores = jnp.einsum('hncd,hnsd->hncs', query_heads * jnp.exp(cum_decay - middle), key_heads * jnp.exp(middle - cum_decay), precision=HIGHEST_PRECISION)
    causal = jnp.tril(jnp.ones((BLK, BLK), dtype=bool))
    scores = jnp.where(causal, scores, 0.0)
    within = jnp.einsum('hncs,hnse->hnce', scores, value_heads, precision=HIGHEST_PRECISION)
    updates = jnp.einsum('hncd,hnce->nhde', key_heads * jnp.exp(block_end - cum_decay), value_heads, precision=HIGHEST_PRECISION)
    block_decay = jnp.exp(block_end[:, :, 0, :]).transpose(1, 0, 2)

    def advance(carry_state, inputs):
        factor, update = inputs
        return (factor[..., None] * carry_state + update, carry_state)
    initial = jnp.zeros((HEADS, HEAD_CHANNELS, HEAD_CHANNELS), jnp.float32)
    _, starts = lax.scan(advance, initial, (block_decay, updates))
    carried = jnp.einsum('hncd,nhde->hnce', query_heads * jnp.exp(cum_decay), starts, precision=HIGHEST_PRECISION)
    return (within + carried).transpose(1, 2, 0, 3).reshape(length, HEADS, HEAD_CHANNELS)

def recurrence_reference(recurrence_query_input, forget_gate_input, recurrence_value_input, output_gate_input, forget_lower_margin, position_decay_extra, head_norm_gain, recurrence_out_weight):
    length = recurrence_query_input.shape[0]
    queries = jax.nn.silu(recurrence_query_input.astype(jnp.float32))
    key_gate_value = forget_lower_margin[None, :] * jax.nn.sigmoid(-forget_gate_input.astype(jnp.float32))
    decay_logarithm = jnp.log1p(-key_gate_value) + jnp.repeat(position_decay_extra, HEAD_CHANNELS, axis=1)
    value_rows = recurrence_value_input.astype(jnp.float32)
    outputs = recurrence(queries, key_gate_value, decay_logarithm, value_rows)
    factor = lax.rsqrt(lax.optimization_barrier(jnp.mean(outputs * outputs, axis=2, keepdims=True)) + EPSILON)
    normed = (outputs * factor).reshape(length, W) * head_norm_gain[None, :]
    gated_rows = (normed * jax.nn.silu(output_gate_input.astype(jnp.float32))).astype(jnp.bfloat16)
    columns = W // N_TP
    summed = jnp.zeros((length, D), jnp.float32)
    for member in range(N_TP):
        partial_sum = jnp.dot(gated_rows[:, member * columns:(member + 1) * columns], recurrence_out_weight[member * columns:(member + 1) * columns], preferred_element_type=jnp.float32).astype(jnp.bfloat16)
        summed = summed + lax.optimization_barrier(partial_sum).astype(jnp.float32)
    return summed.astype(jnp.bfloat16)

def expert_reference(expert_hidden_state, chosen_expert_index, chosen_expert_score, expert_norm_gain, routed_gate_weight, routed_up_weight, routed_down_weight, shared_gate_weight, shared_up_weight, shared_down_weight):
    tokens = expert_hidden_state.shape[0]
    features = expert_hidden_state.astype(jnp.float32)
    normed = (features * lax.rsqrt(lax.optimization_barrier(jnp.mean(features * features, axis=1, keepdims=True)) + EPSILON) * expert_norm_gain[None, :]).astype(jnp.bfloat16)
    gates = ROUTED_SCALE * chosen_expert_score / lax.optimization_barrier(jnp.sum(chosen_expert_score, axis=1, keepdims=True))
    blocked = chosen_expert_index.reshape(N_EP, TOKB_DEV * TOP_K)
    onehot = (blocked[:, :, None] == jnp.arange(EXPERTS, dtype=jnp.int32)[None, None, :]).astype(jnp.int32)
    places = lax.optimization_barrier(jnp.sum(onehot * (jnp.cumsum(onehot, axis=1) - 1), axis=2)).reshape(-1)
    sources = jnp.arange(tokens * TOP_K, dtype=jnp.int32) // (TOKB_DEV * TOP_K)
    slots = (chosen_expert_index.reshape(-1) * N_EP + sources) * CAP + places
    owners = jnp.full((EXPERTS * N_EP * CAP,), tokens, jnp.int32).at[slots].set(jnp.arange(tokens * TOP_K, dtype=jnp.int32) // TOP_K)
    padded = jnp.concatenate([normed, jnp.zeros((1, D), jnp.bfloat16)], axis=0)
    grouped = padded[owners].reshape(EXPERTS, N_EP * CAP, D)

    def one_expert(inputs):
        slot_rows, gate_matrix, up_matrix, down_matrix = inputs
        hidden = (jax.nn.silu(jnp.dot(slot_rows, gate_matrix, preferred_element_type=jnp.float32)) * jnp.dot(slot_rows, up_matrix, preferred_element_type=jnp.float32)).astype(jnp.bfloat16)
        return jnp.dot(hidden, down_matrix, preferred_element_type=jnp.float32).astype(jnp.bfloat16)
    results = lax.map(one_expert, (grouped, routed_gate_weight, routed_up_weight, routed_down_weight))
    picked = results.reshape(EXPERTS * N_EP * CAP, D)[slots].reshape(tokens, TOP_K, D)
    shared_hidden = (jax.nn.silu(jnp.dot(normed, shared_gate_weight, preferred_element_type=jnp.float32)) * jnp.dot(normed, shared_up_weight, preferred_element_type=jnp.float32)).astype(jnp.bfloat16)
    shared_result = jnp.dot(shared_hidden, shared_down_weight, preferred_element_type=jnp.float32)
    combined = shared_result + lax.optimization_barrier(jnp.sum(gates[:, :, None] * picked.astype(jnp.float32), axis=1))
    return combined.astype(jnp.bfloat16)

def reference(recurrence_query_input, forget_gate_input, recurrence_value_input, output_gate_input, forget_lower_margin, position_decay_extra, head_norm_gain, recurrence_out_weight, expert_hidden_state, chosen_expert_index, chosen_expert_score, expert_norm_gain, routed_gate_weight, routed_up_weight, routed_down_weight, shared_gate_weight, shared_up_weight, shared_down_weight):
    recurrence_output = recurrence_reference(recurrence_query_input, forget_gate_input, recurrence_value_input, output_gate_input, forget_lower_margin, position_decay_extra, head_norm_gain, recurrence_out_weight)
    expert_out = expert_reference(expert_hidden_state, chosen_expert_index, chosen_expert_score, expert_norm_gain, routed_gate_weight, routed_up_weight, routed_down_weight, shared_gate_weight, shared_up_weight, shared_down_weight)
    return (recurrence_output, expert_out)
```

```python
import jax
import jax.numpy as jnp
from jax import lax
from jax.sharding import PartitionSpec as P

HEAD_CHANNELS = 128
BLK = 64


EPSILON = 1e-06
ROUTED_SCALE = 2.5
PRECISION = lax.Precision.DEFAULT


def carried_in(array, axis, combine, identity):
    count, index = (lax.axis_size(axis), lax.axis_index(axis))
    everything = jax.tree.map(
        lambda part, kind: lax.all_gather(part.astype(kind), axis),
        array,
        (jnp.bfloat16, jnp.bfloat16),
    )
    start = jax.tree.map(
        lambda part, zero: jnp.broadcast_to(jnp.asarray(zero, part.dtype), part.shape),
        array,
        identity,
    )

    def turn(k, before):
        reached = k < index
        new = combine(
            before, jax.tree.map(lambda part, own: part[k].astype(own.dtype), everything, array)
        )
        return jax.tree.map(lambda a, b: jnp.where(reached, a, b), new, before)

    return lax.fori_loop(0, count, turn, start)


def chain_states(earlier, later):
    return (earlier[0] * later[0], later[0][..., None] * earlier[1] + later[1])


def mixer_half(
    recurrence_query_input,
    forget_gate_input,
    recurrence_value_input,
    output_gate_input,
    forget_lower_margin,
    position_decay_extra,
    head_norm_gain,
    recurrence_out_weight,
):
    length = recurrence_query_input.shape[0]
    head_tensor = position_decay_extra.shape[1]
    blocks = length // BLK
    queries = jax.nn.silu(recurrence_query_input.astype(jnp.float32))
    key_gate_value = forget_lower_margin[None, :] * jax.nn.sigmoid(
        -forget_gate_input.astype(jnp.float32)
    )
    decay_logarithm = jnp.log1p(-key_gate_value) + jnp.repeat(
        position_decay_extra, HEAD_CHANNELS, axis=1
    )
    value_rows = recurrence_value_input.astype(jnp.float32)

    def split_heads(tensor):
        return tensor.reshape(blocks, BLK, head_tensor, HEAD_CHANNELS).transpose(2, 0, 1, 3)

    query_heads = split_heads(queries)
    key_heads = split_heads(key_gate_value)
    value_heads = split_heads(value_rows)
    cum_decay = jnp.cumsum(split_heads(decay_logarithm), axis=2)
    middle = cum_decay[:, :, BLK // 2 - 1 : BLK // 2]
    block_end = cum_decay[:, :, BLK - 1 : BLK]
    scores = jnp.einsum(
        "hncd,hnsd->hncs",
        query_heads * jnp.exp(cum_decay - middle),
        key_heads * jnp.exp(middle - cum_decay),
        precision=PRECISION,
    )
    causal = jnp.tril(jnp.ones((BLK, BLK), dtype=bool))
    scores = jnp.where(causal, scores, 0.0)
    within = jnp.einsum("hncs,hnse->hnce", scores, value_heads, precision=PRECISION)
    updates = jnp.einsum(
        "hncd,hnce->nhde",
        key_heads * jnp.exp(block_end - cum_decay),
        value_heads,
        precision=PRECISION,
    )
    block_log = block_end[:, :, 0, :]
    block_decay = jnp.exp(block_log).transpose(1, 0, 2)

    def advance(carry_state, inputs):
        factor, update = inputs
        return (factor[..., None] * carry_state + update, carry_state)

    initial = jnp.zeros((head_tensor, HEAD_CHANNELS, HEAD_CHANNELS), jnp.float32)
    local_final, local_starts = lax.scan(advance, initial, (block_decay, updates))
    device_decay = jnp.exp(jnp.sum(block_log, axis=1))
    identity = (jnp.ones_like(device_decay), jnp.zeros_like(local_final))
    _, incoming = carried_in((device_decay, local_final), "ep", chain_states, identity)
    before = jnp.exp(jnp.cumsum(block_log, axis=1) - block_log).transpose(1, 0, 2)
    starts = local_starts + before[..., None] * incoming[None]
    carried = jnp.einsum(
        "hncd,nhde->hnce", query_heads * jnp.exp(cum_decay), starts, precision=PRECISION
    )
    outputs = (within + carried).transpose(1, 2, 0, 3).reshape(length, head_tensor, HEAD_CHANNELS)
    factor = lax.rsqrt(jnp.mean(outputs * outputs, axis=2, keepdims=True) + EPSILON)
    normed = (outputs * factor).reshape(length, head_tensor * HEAD_CHANNELS) * head_norm_gain[
        None, :
    ]
    gated_rows = (normed * jax.nn.silu(output_gate_input.astype(jnp.float32))).astype(jnp.bfloat16)
    return lax.psum_scatter(
        jnp.dot(gated_rows, recurrence_out_weight, preferred_element_type=jnp.float32).astype(
            jnp.bfloat16
        ),
        "tp",
        scatter_dimension=0,
        tiled=True,
    )


def expert_half(
    expert_hidden_state,
    chosen_expert_index,
    chosen_expert_score,
    expert_norm_gain,
    routed_gate_weight,
    routed_up_weight,
    routed_down_weight,
    shared_gate_weight,
    shared_up_weight,
    shared_down_weight,
):
    tokens, top = chosen_expert_index.shape
    local_experts = routed_gate_weight.shape[0]
    devices = lax.axis_size("ep")
    experts = local_experts * devices
    capacity = min(tokens, 2 * tokens * top // experts)
    width_out = routed_down_weight.shape[2]
    features = expert_hidden_state.astype(jnp.float32)
    normed = (
        features
        * lax.rsqrt(jnp.mean(features * features, axis=1, keepdims=True) + EPSILON)
        * expert_norm_gain[None, :]
    ).astype(jnp.bfloat16)
    gates = ROUTED_SCALE * chosen_expert_score / jnp.sum(chosen_expert_score, axis=1, keepdims=True)
    flat_ids = chosen_expert_index.reshape(-1)
    onehot = (flat_ids[:, None] == jnp.arange(experts, dtype=jnp.int32)[None, :]).astype(jnp.int32)
    places = jnp.sum(onehot * (jnp.cumsum(onehot, axis=0) - 1), axis=1)
    slots = flat_ids * capacity + places
    owners = (
        jnp.full((experts * capacity,), tokens, jnp.int32)
        .at[slots]
        .set(jnp.arange(tokens * top, dtype=jnp.int32) // top)
    )
    padded = jnp.concatenate([normed, jnp.zeros((1, normed.shape[1]), jnp.bfloat16)], axis=0)
    outgoing = padded[owners].reshape(experts, capacity, normed.shape[1])
    piece = lax.all_to_all(outgoing, "ep", split_axis=0, concat_axis=0, tiled=True)
    grouped = piece.reshape(devices, local_experts, piece.shape[1], piece.shape[2])
    gate_part = jnp.einsum(
        "secd,edh->sech", grouped, routed_gate_weight, preferred_element_type=jnp.float32
    )
    up_part = jnp.einsum(
        "secd,edh->sech", grouped, routed_up_weight, preferred_element_type=jnp.float32
    )
    hidden = (jax.nn.silu(gate_part) * up_part).astype(jnp.bfloat16)
    hidden_rows = hidden.reshape(devices * local_experts, piece.shape[1], hidden.shape[3])
    flat_hidden = hidden_rows.reshape(experts * capacity, hidden_rows.shape[2])
    shared_hidden = (
        jax.nn.silu(jnp.dot(normed, shared_gate_weight, preferred_element_type=jnp.float32))
        * jnp.dot(normed, shared_up_weight, preferred_element_type=jnp.float32)
    ).astype(jnp.bfloat16)
    start_values = (
        jnp.zeros((experts * capacity, width_out), jnp.float32),
        jnp.zeros((tokens, width_out), jnp.float32),
    )
    routed_piece = lax.all_gather(flat_hidden, "tp", axis=1, tiled=True)
    shared_piece = lax.all_gather(shared_hidden, "tp", axis=1, tiled=True)
    count = routed_piece.shape[1]
    grouped = routed_piece.reshape(devices, local_experts, capacity, count)
    routed = jnp.einsum(
        "secn,enk->seck", grouped, routed_down_weight, preferred_element_type=jnp.float32
    )
    shared = jnp.dot(shared_piece, shared_down_weight, preferred_element_type=jnp.float32)
    routed_sum = routed.reshape(start_values[0].shape)
    answers = routed_sum.astype(jnp.bfloat16).reshape(experts, capacity, width_out)
    returned = lax.all_to_all(answers, "ep", split_axis=0, concat_axis=0, tiled=True)
    picked_rows = returned.reshape(experts * capacity, width_out)[slots].reshape(
        tokens, top, width_out
    )
    combined = shared + jnp.sum(gates[:, :, None] * picked_rows.astype(jnp.float32), axis=1)
    return combined.astype(jnp.bfloat16)


def dense_expert_half(
    expert_hidden_state,
    chosen_expert_index,
    chosen_expert_score,
    expert_norm_gain,
    routed_gate_weight,
    routed_up_weight,
    routed_down_weight,
    shared_gate_weight,
    shared_up_weight,
    shared_down_weight,
):
    tokens, top = chosen_expert_index.shape
    experts = lax.axis_size("ep")
    features = expert_hidden_state.astype(jnp.float32)
    width = features.shape[1]
    normed = (
        features
        * lax.rsqrt(jnp.mean(features * features, axis=1, keepdims=True) + EPSILON)
        * expert_norm_gain[None, :]
    ).astype(jnp.bfloat16)
    gates = ROUTED_SCALE * chosen_expert_score / jnp.sum(chosen_expert_score, axis=1, keepdims=True)
    chosen = chosen_expert_index[:, :, None] == jnp.arange(64, dtype=jnp.int32)[None, None, :]
    gate_table = jnp.sum(jnp.where(chosen, gates[:, :, None], 0.0), axis=1)
    high = gate_table.astype(jnp.bfloat16)
    low = (gate_table - high.astype(jnp.float32)).astype(jnp.bfloat16)
    sent = jnp.concatenate([normed, high, low], axis=1)
    everything = lax.all_gather(sent, "ep", axis=0, tiled=True)
    rows = everything[:, :width]
    mine = jnp.arange(64, dtype=jnp.int32) == lax.axis_index("ep")
    tail = everything[:, width:].astype(jnp.float32)
    own_gate = jnp.sum(jnp.where(mine[None, :], tail[:, :64] + tail[:, 64:], 0.0), axis=1)
    shared_hidden = (
        jax.nn.silu(jnp.dot(normed, shared_gate_weight, preferred_element_type=jnp.float32))
        * jnp.dot(normed, shared_up_weight, preferred_element_type=jnp.float32)
    ).astype(jnp.bfloat16)
    gate_part = jnp.dot(rows, routed_gate_weight[0], preferred_element_type=jnp.float32)
    up_part = jnp.dot(rows, routed_up_weight[0], preferred_element_type=jnp.float32)
    hidden = (jax.nn.silu(gate_part) * up_part * own_gate[:, None]).astype(jnp.bfloat16)
    shared_full = lax.all_gather(shared_hidden, "tp", axis=1, tiled=True)
    hidden_full = lax.all_gather(hidden, "tp", axis=1, tiled=True)
    shared = jnp.dot(shared_full, shared_down_weight, preferred_element_type=jnp.float32)
    routed = jnp.dot(
        hidden_full, routed_down_weight[0], preferred_element_type=jnp.float32
    ).astype(jnp.bfloat16)
    total = lax.psum_scatter(routed, "ep", scatter_dimension=0, tiled=True)
    return (shared + total.astype(jnp.float32)).astype(jnp.bfloat16)


def per_device(
    recurrence_query_input,
    forget_gate_input,
    recurrence_value_input,
    output_gate_input,
    forget_lower_margin,
    position_decay_extra,
    head_norm_gain,
    recurrence_out_weight,
    expert_hidden_state,
    chosen_expert_index,
    chosen_expert_score,
    expert_norm_gain,
    routed_gate_weight,
    routed_up_weight,
    routed_down_weight,
    shared_gate_weight,
    shared_up_weight,
    shared_down_weight,
):
    recurrence_output = mixer_half(
        recurrence_query_input,
        forget_gate_input,
        recurrence_value_input,
        output_gate_input,
        forget_lower_margin,
        position_decay_extra,
        head_norm_gain,
        recurrence_out_weight,
    )
    tokens, top = chosen_expert_index.shape
    experts = routed_gate_weight.shape[0] * lax.axis_size("ep")
    every_row_fits = 2 * top >= experts and routed_gate_weight.shape[0] == 1 and experts <= 64
    half = dense_expert_half if every_row_fits else expert_half
    expert_out = half(
        expert_hidden_state,
        chosen_expert_index,
        chosen_expert_score,
        expert_norm_gain,
        routed_gate_weight,
        routed_up_weight,
        routed_down_weight,
        shared_gate_weight,
        shared_up_weight,
        shared_down_weight,
    )
    return (recurrence_output, expert_out)


def solution(mesh):
    in_specs = (
        P(("grp", "ep"), "tp"),
        P(("grp", "ep"), "tp"),
        P(("grp", "ep"), "tp"),
        P(("grp", "ep"), "tp"),
        P("tp"),
        P(("grp", "ep"), "tp"),
        P("tp"),
        P("tp", None),
        P(("grp", "ep"), None),
        P(("grp", "ep"), None),
        P(("grp", "ep"), None),
        P(),
        P("ep", None, "tp"),
        P("ep", None, "tp"),
        P("ep", None, "tp"),
        P(None, "tp"),
        P(None, "tp"),
        P(None, "tp"),
    )
    out_specs = (P(("grp", "ep", "tp"), None), P(("grp", "ep"), "tp"))
    return jax.shard_map(
        per_device, mesh=mesh, in_specs=in_specs, out_specs=out_specs, check_vma=False
    )
```

```python
import functools

import jax
import jax.numpy as jnp
from jax import lax
from jax.experimental import pallas as pl
from jax.experimental.pallas import tpu as pltpu
from jax.sharding import PartitionSpec as P

HEAD_CHANNELS = 128
BLK = 64


EPSILON = 1e-06
ROUTED_SCALE = 2.5
PRECISION = lax.Precision.DEFAULT


def carried_in(array, axis, combine, identity):
    count, index = (lax.axis_size(axis), lax.axis_index(axis))
    everything = jax.tree.map(
        lambda part, kind: lax.all_gather(part.astype(kind), axis),
        array,
        (jnp.bfloat16, jnp.bfloat16),
    )
    start = jax.tree.map(
        lambda part, zero: jnp.broadcast_to(jnp.asarray(zero, part.dtype), part.shape),
        array,
        identity,
    )

    def turn(k, before):
        reached = k < index
        new = combine(
            before, jax.tree.map(lambda part, own: part[k].astype(own.dtype), everything, array)
        )
        return jax.tree.map(lambda a, b: jnp.where(reached, a, b), new, before)

    return lax.fori_loop(0, count, turn, start)


def chain_states(earlier, later):
    return (earlier[0] * later[0], later[0][..., None] * earlier[1] + later[1])


def mixer_half(
    recurrence_query_input,
    forget_gate_input,
    recurrence_value_input,
    output_gate_input,
    forget_lower_margin,
    position_decay_extra,
    head_norm_gain,
    recurrence_out_weight,
):
    length = recurrence_query_input.shape[0]
    head_tensor = position_decay_extra.shape[1]
    blocks = length // BLK
    queries = jax.nn.silu(recurrence_query_input.astype(jnp.float32))
    key_gate_value = forget_lower_margin[None, :] * jax.nn.sigmoid(
        -forget_gate_input.astype(jnp.float32)
    )
    decay_logarithm = jnp.log1p(-key_gate_value) + jnp.repeat(
        position_decay_extra, HEAD_CHANNELS, axis=1
    )
    value_rows = recurrence_value_input.astype(jnp.float32)

    def split_heads(tensor):
        return tensor.reshape(blocks, BLK, head_tensor, HEAD_CHANNELS).transpose(2, 0, 1, 3)

    query_heads = split_heads(queries)
    key_heads = split_heads(key_gate_value)
    value_heads = split_heads(value_rows)
    cum_decay = jnp.cumsum(split_heads(decay_logarithm), axis=2)
    middle = cum_decay[:, :, BLK // 2 - 1 : BLK // 2]
    block_end = cum_decay[:, :, BLK - 1 : BLK]
    scores = jnp.einsum(
        "hncd,hnsd->hncs",
        query_heads * jnp.exp(cum_decay - middle),
        key_heads * jnp.exp(middle - cum_decay),
        precision=PRECISION,
    )
    causal = jnp.tril(jnp.ones((BLK, BLK), dtype=bool))
    scores = jnp.where(causal, scores, 0.0)
    within = jnp.einsum("hncs,hnse->hnce", scores, value_heads, precision=PRECISION)
    updates = jnp.einsum(
        "hncd,hnce->nhde",
        key_heads * jnp.exp(block_end - cum_decay),
        value_heads,
        precision=PRECISION,
    )
    block_log = block_end[:, :, 0, :]
    block_decay = jnp.exp(block_log).transpose(1, 0, 2)

    def advance(carry_state, inputs):
        factor, update = inputs
        return (factor[..., None] * carry_state + update, carry_state)

    initial = jnp.zeros((head_tensor, HEAD_CHANNELS, HEAD_CHANNELS), jnp.float32)
    local_final, local_starts = lax.scan(advance, initial, (block_decay, updates))
    device_decay = jnp.exp(jnp.sum(block_log, axis=1))
    identity = (jnp.ones_like(device_decay), jnp.zeros_like(local_final))
    _, incoming = carried_in((device_decay, local_final), "ep", chain_states, identity)
    before = jnp.exp(jnp.cumsum(block_log, axis=1) - block_log).transpose(1, 0, 2)
    starts = local_starts + before[..., None] * incoming[None]
    carried = jnp.einsum(
        "hncd,nhde->hnce", query_heads * jnp.exp(cum_decay), starts, precision=PRECISION
    )
    outputs = (within + carried).transpose(1, 2, 0, 3).reshape(length, head_tensor, HEAD_CHANNELS)
    factor = lax.rsqrt(jnp.mean(outputs * outputs, axis=2, keepdims=True) + EPSILON)
    normed = (outputs * factor).reshape(length, head_tensor * HEAD_CHANNELS) * head_norm_gain[
        None, :
    ]
    gated_rows = (normed * jax.nn.silu(output_gate_input.astype(jnp.float32))).astype(jnp.bfloat16)
    return lax.psum_scatter(
        jnp.dot(gated_rows, recurrence_out_weight, preferred_element_type=jnp.float32).astype(
            jnp.bfloat16
        ),
        "tp",
        scatter_dimension=0,
        tiled=True,
    )


def expert_half(
    expert_hidden_state,
    chosen_expert_index,
    chosen_expert_score,
    expert_norm_gain,
    routed_gate_weight,
    routed_up_weight,
    routed_down_weight,
    shared_gate_weight,
    shared_up_weight,
    shared_down_weight,
):
    tokens, top = chosen_expert_index.shape
    local_experts = routed_gate_weight.shape[0]
    devices = lax.axis_size("ep")
    experts = local_experts * devices
    capacity = min(tokens, 2 * tokens * top // experts)
    width_out = routed_down_weight.shape[2]
    features = expert_hidden_state.astype(jnp.float32)
    normed = (
        features
        * lax.rsqrt(jnp.mean(features * features, axis=1, keepdims=True) + EPSILON)
        * expert_norm_gain[None, :]
    ).astype(jnp.bfloat16)
    gates = ROUTED_SCALE * chosen_expert_score / jnp.sum(chosen_expert_score, axis=1, keepdims=True)
    flat_ids = chosen_expert_index.reshape(-1)
    onehot = (flat_ids[:, None] == jnp.arange(experts, dtype=jnp.int32)[None, :]).astype(jnp.int32)
    places = jnp.sum(onehot * (jnp.cumsum(onehot, axis=0) - 1), axis=1)
    slots = flat_ids * capacity + places
    owners = (
        jnp.full((experts * capacity,), tokens, jnp.int32)
        .at[slots]
        .set(jnp.arange(tokens * top, dtype=jnp.int32) // top)
    )
    padded = jnp.concatenate([normed, jnp.zeros((1, normed.shape[1]), jnp.bfloat16)], axis=0)
    outgoing = padded[owners].reshape(experts, capacity, normed.shape[1])
    piece = lax.all_to_all(outgoing, "ep", split_axis=0, concat_axis=0, tiled=True)
    grouped = piece.reshape(devices, local_experts, piece.shape[1], piece.shape[2])
    gate_part = jnp.einsum(
        "secd,edh->sech", grouped, routed_gate_weight, preferred_element_type=jnp.float32
    )
    up_part = jnp.einsum(
        "secd,edh->sech", grouped, routed_up_weight, preferred_element_type=jnp.float32
    )
    hidden = (jax.nn.silu(gate_part) * up_part).astype(jnp.bfloat16)
    hidden_rows = hidden.reshape(devices * local_experts, piece.shape[1], hidden.shape[3])
    flat_hidden = hidden_rows.reshape(experts * capacity, hidden_rows.shape[2])
    shared_hidden = (
        jax.nn.silu(jnp.dot(normed, shared_gate_weight, preferred_element_type=jnp.float32))
        * jnp.dot(normed, shared_up_weight, preferred_element_type=jnp.float32)
    ).astype(jnp.bfloat16)
    start_values = (
        jnp.zeros((experts * capacity, width_out), jnp.float32),
        jnp.zeros((tokens, width_out), jnp.float32),
    )
    routed_piece = lax.all_gather(flat_hidden, "tp", axis=1, tiled=True)
    shared_piece = lax.all_gather(shared_hidden, "tp", axis=1, tiled=True)
    count = routed_piece.shape[1]
    grouped = routed_piece.reshape(devices, local_experts, capacity, count)
    routed = jnp.einsum(
        "secn,enk->seck", grouped, routed_down_weight, preferred_element_type=jnp.float32
    )
    shared = jnp.dot(shared_piece, shared_down_weight, preferred_element_type=jnp.float32)
    routed_sum = routed.reshape(start_values[0].shape)
    answers = routed_sum.astype(jnp.bfloat16).reshape(experts, capacity, width_out)
    returned = lax.all_to_all(answers, "ep", split_axis=0, concat_axis=0, tiled=True)
    picked_rows = returned.reshape(experts * capacity, width_out)[slots].reshape(
        tokens, top, width_out
    )
    combined = shared + jnp.sum(gates[:, :, None] * picked_rows.astype(jnp.float32), axis=1)
    return combined.astype(jnp.bfloat16)


MESH = pl.DeviceIdType.MESH
LANES = 128


def expert_kernel(
    count,
    x_ref,
    gate_hbm,
    up_hbm,
    down_hbm,
    shared_gate_hbm,
    shared_up_hbm,
    shared_down_hbm,
    routed_ref,
    shared_ref,
    rows,
    gate_w,
    up_w,
    down_w,
    shared_gate_w,
    shared_up_w,
    shared_down_w,
    own_hidden,
    peer_hidden,
    load_sem,
    right_sem,
    left_sem,
    side_sem,
    row_sem,
    hidden_send,
    hidden_recv,
):
    chips = count // 2
    me = lax.axis_index("ep")
    half = lax.axis_index("tp")
    chip, core = me // 2, me % 2
    side = chip * 2 + 1 - core
    partner = 1 - half
    block_rows = x_ref.shape[0]
    width = gate_w.shape[0]
    units = gate_w.shape[1]
    has_right, has_left = chip < chips - 1, chip > 0

    def half_rows(ref, which):
        return ref.at[pl.ds(pl.multiple_of(which * units, units), units), :]

    loads = [
        (shared_gate_hbm, shared_gate_w),
        (shared_up_hbm, shared_up_w),
        (gate_hbm.at[0], gate_w),
        (up_hbm.at[0], up_w),
        (half_rows(down_hbm.at[0], half), down_w.at[0]),
        (half_rows(down_hbm.at[0], partner), down_w.at[1]),
        (half_rows(shared_down_hbm, half), shared_down_w.at[0]),
        (half_rows(shared_down_hbm, partner), shared_down_w.at[1]),
        (x_ref, rows.at[me]),
    ]
    copies = [
        pltpu.make_async_copy(source, target, load_sem.at[i])
        for i, (source, target) in enumerate(loads)
    ]
    for copy in copies:
        copy.start()

    barrier = pltpu.get_barrier_semaphore()
    pl.semaphore_signal(barrier, inc=1, device_id={"ep": side}, device_id_type=MESH)
    pl.semaphore_signal(barrier, inc=1, device_id={"tp": partner}, device_id_type=MESH)

    @pl.when(has_right)
    def _():
        pl.semaphore_signal(barrier, inc=1, device_id={"ep": me + 2}, device_id_type=MESH)

    @pl.when(has_left)
    def _():
        pl.semaphore_signal(barrier, inc=1, device_id={"ep": me - 2}, device_id_type=MESH)

    pl.semaphore_wait(barrier, 2 + has_right.astype(jnp.int32) + has_left.astype(jnp.int32))

    def row_copy(source, block, sems, target):
        return pltpu.make_async_remote_copy(
            src_ref=source,
            dst_ref=rows.at[block],
            send_sem=sems.at[block],
            recv_sem=row_sem.at[block],
            device_id={"ep": target},
            device_id_type=MESH,
        )

    def hidden_copy(step):
        return pltpu.make_async_remote_copy(
            src_ref=own_hidden.at[step],
            dst_ref=peer_hidden.at[step],
            send_sem=hidden_send.at[step],
            recv_sem=hidden_recv.at[step],
            device_id={"tp": partner},
            device_id_type=MESH,
        )

    def block_of(step):
        k, odd = step // 2, step % 2
        inner = jnp.minimum(chip, chips - 1 - chip)
        near = jnp.where(k % 2 == 1, chip - (k + 1) // 2, chip + k // 2)
        far = jnp.where(chip <= chips - 1 - chip, k, chips - 1 - k)
        source = jnp.where(k <= 2 * inner, near, far)
        return source, source * 2 + jnp.where(odd == 1, 1 - core, core)

    def goes_right(source):
        return jnp.logical_and(source <= chip, has_right)

    def goes_left(source):
        return jnp.logical_and(source >= chip, has_left)

    @pl.when(has_right)
    def _():
        row_copy(x_ref, me, right_sem, me + 2).start()

    @pl.when(has_left)
    def _():
        row_copy(x_ref, me, left_sem, me - 2).start()

    row_copy(x_ref, me, side_sem, side).start()

    copies[0].wait()
    copies[1].wait()
    gate_part = jnp.dot(
        x_ref[:, :width], shared_gate_w[...], preferred_element_type=jnp.float32
    )
    up_part = jnp.dot(x_ref[:, :width], shared_up_w[...], preferred_element_type=jnp.float32)
    own_hidden[count] = (jax.nn.silu(gate_part) * up_part).astype(jnp.bfloat16)
    for copy in copies[2:]:
        copy.wait()

    def down(step, weight):
        hidden_copy(step).wait_recv()
        return jnp.dot(
            own_hidden[step], weight[0], preferred_element_type=jnp.float32
        ) + jnp.dot(peer_hidden[step], weight[1], preferred_element_type=jnp.float32)

    def routed_down(step):
        _, block = block_of(step)
        place = pl.ds(pl.multiple_of(block * block_rows, block_rows), block_rows)
        routed_ref[place, :] = down(step, down_w).astype(jnp.bfloat16)

    def turn(step, _):
        source, block = block_of(step)
        odd = step % 2

        @pl.when(step > 0)
        def _():
            row_copy(x_ref, block, side_sem, side).wait_recv()

        @pl.when(jnp.logical_and(step > 0, odd == 0))
        def _():
            @pl.when(goes_right(source))
            def _():
                row_copy(rows.at[block], block, right_sem, me + 2).start()

            @pl.when(goes_left(source))
            def _():
                row_copy(rows.at[block], block, left_sem, me - 2).start()

            row_copy(rows.at[block], block, side_sem, side).start()

        x = rows[block, :, :width]
        tail = rows[block, :, width:].astype(jnp.float32)
        lane = lax.broadcasted_iota(jnp.int32, tail.shape, 1)
        own_gate = jnp.sum(
            jnp.where(lane % (LANES // 2) == me, tail, 0.0), axis=1, keepdims=True
        )
        gate_part = jnp.dot(x, gate_w[...], preferred_element_type=jnp.float32)
        up_part = jnp.dot(x, up_w[...], preferred_element_type=jnp.float32)
        own_hidden[step] = (jax.nn.silu(gate_part) * up_part * own_gate).astype(jnp.bfloat16)

        @pl.when(step == 0)
        def _():
            hidden_copy(count).start()

        @pl.when(step > 0)
        def _():
            routed_down(step - 1)

        hidden_copy(step).start()
        return 0

    lax.fori_loop(0, count, turn, 0)
    shared_ref[...] = down(count, shared_down_w)
    routed_down(count - 1)

    def finish(step, _):
        source, block = block_of(step)
        hidden_copy(step).wait_send()

        @pl.when(step % 2 == 0)
        def _():
            @pl.when(goes_right(source))
            def _():
                row_copy(x_ref, block, right_sem, me + 2).wait_send()

            @pl.when(goes_left(source))
            def _():
                row_copy(x_ref, block, left_sem, me - 2).wait_send()

            row_copy(x_ref, block, side_sem, side).wait_send()

        return 0

    lax.fori_loop(0, count, finish, 0)
    hidden_copy(count).wait_send()


def dense_expert_half(
    expert_hidden_state,
    chosen_expert_index,
    chosen_expert_score,
    expert_norm_gain,
    routed_gate_weight,
    routed_up_weight,
    routed_down_weight,
    shared_gate_weight,
    shared_up_weight,
    shared_down_weight,
):
    tokens = chosen_expert_index.shape[0]
    count = lax.axis_size("ep")
    features = expert_hidden_state.astype(jnp.float32)
    width = features.shape[1]
    units, width_out = routed_gate_weight.shape[2], routed_down_weight.shape[2]
    normed = (
        features
        * lax.rsqrt(jnp.mean(features * features, axis=1, keepdims=True) + EPSILON)
        * expert_norm_gain[None, :]
    ).astype(jnp.bfloat16)
    gates = ROUTED_SCALE * chosen_expert_score / jnp.sum(chosen_expert_score, axis=1, keepdims=True)
    slots = LANES // 2
    chosen = chosen_expert_index[:, :, None] == jnp.arange(slots, dtype=jnp.int32)[None, None, :]
    gate_table = jnp.sum(jnp.where(chosen, gates[:, :, None], 0.0), axis=1)
    high = gate_table.astype(jnp.bfloat16)
    low = (gate_table - high.astype(jnp.float32)).astype(jnp.bfloat16)
    sent = jnp.concatenate([normed, high, low], axis=1)
    hbm = pl.BlockSpec(memory_space=pl.ANY)
    vmem = pl.BlockSpec(memory_space=pltpu.VMEM)
    weight = pltpu.VMEM((width, units), jnp.bfloat16)
    down_weight = pltpu.VMEM((2, units, width_out), jnp.bfloat16)
    hidden = pltpu.VMEM((count + 1, tokens, units), jnp.bfloat16)
    block_sems = pltpu.SemaphoreType.DMA((count,))
    routed, shared = pl.pallas_call(
        functools.partial(expert_kernel, count),
        out_shape=(
            jax.ShapeDtypeStruct((count * tokens, width_out), jnp.bfloat16),
            jax.ShapeDtypeStruct((tokens, width_out), jnp.float32),
        ),
        in_specs=[vmem] + [hbm] * 6,
        out_specs=(vmem, vmem),
        scratch_shapes=[
            pltpu.VMEM((count, tokens, width + LANES), jnp.bfloat16),
            weight,
            weight,
            down_weight,
            weight,
            weight,
            down_weight,
            hidden,
            hidden,
            pltpu.SemaphoreType.DMA((9,)),
            block_sems,
            block_sems,
            block_sems,
            block_sems,
            pltpu.SemaphoreType.DMA((count + 1,)),
            pltpu.SemaphoreType.DMA((count + 1,)),
        ],
        compiler_params=pltpu.CompilerParams(
            collective_id=0, has_side_effects=True, vmem_limit_bytes=48 * 1024 * 1024
        ),
        cost_estimate=pl.CostEstimate(
            flops=45_000_000_000, bytes_accessed=16_000_000, transcendentals=0
        ),
        name="expert_kernel",
    )(
        sent,
        routed_gate_weight,
        routed_up_weight,
        routed_down_weight,
        shared_gate_weight,
        shared_up_weight,
        shared_down_weight,
    )
    total = lax.psum_scatter(routed, "ep", scatter_dimension=0, tiled=True)
    return (shared + total.astype(jnp.float32)).astype(jnp.bfloat16)


def per_device(
    recurrence_query_input,
    forget_gate_input,
    recurrence_value_input,
    output_gate_input,
    forget_lower_margin,
    position_decay_extra,
    head_norm_gain,
    recurrence_out_weight,
    expert_hidden_state,
    chosen_expert_index,
    chosen_expert_score,
    expert_norm_gain,
    routed_gate_weight,
    routed_up_weight,
    routed_down_weight,
    shared_gate_weight,
    shared_up_weight,
    shared_down_weight,
):
    recurrence_output = mixer_half(
        recurrence_query_input,
        forget_gate_input,
        recurrence_value_input,
        output_gate_input,
        forget_lower_margin,
        position_decay_extra,
        head_norm_gain,
        recurrence_out_weight,
    )
    tokens, top = chosen_expert_index.shape
    experts = routed_gate_weight.shape[0] * lax.axis_size("ep")
    every_row_fits = 2 * top >= experts and routed_gate_weight.shape[0] == 1 and experts <= 64
    half = dense_expert_half if every_row_fits else expert_half
    expert_out = half(
        expert_hidden_state,
        chosen_expert_index,
        chosen_expert_score,
        expert_norm_gain,
        routed_gate_weight,
        routed_up_weight,
        routed_down_weight,
        shared_gate_weight,
        shared_up_weight,
        shared_down_weight,
    )
    return (recurrence_output, expert_out)


def solution(mesh):
    in_specs = (
        P(("grp", "ep"), "tp"),
        P(("grp", "ep"), "tp"),
        P(("grp", "ep"), "tp"),
        P(("grp", "ep"), "tp"),
        P("tp"),
        P(("grp", "ep"), "tp"),
        P("tp"),
        P("tp", None),
        P(("grp", "ep"), None),
        P(("grp", "ep"), None),
        P(("grp", "ep"), None),
        P(),
        P("ep", None, "tp"),
        P("ep", None, "tp"),
        P("ep", None, "tp"),
        P(None, "tp"),
        P(None, "tp"),
        P(None, "tp"),
    )
    out_specs = (P(("grp", "ep", "tp"), None), P(("grp", "ep"), "tp"))
    return jax.shard_map(
        per_device, mesh=mesh, in_specs=in_specs, out_specs=out_specs, check_vma=False
    )
```

```python
import functools

import jax
import jax.numpy as jnp
from jax import lax
from jax.experimental import pallas as pl
from jax.experimental.pallas import tpu as pltpu
from jax.sharding import PartitionSpec as P

HEAD_CHANNELS = 128
BLK = 64


EPSILON = 1e-06
ROUTED_SCALE = 2.5
PRECISION = lax.Precision.DEFAULT


DECAY_ROWS = 16


def carried_in(decay, state, axis):
    count, index = (lax.axis_size(axis), lax.axis_index(axis))
    depth = state.shape[1]
    rows = jnp.broadcast_to(decay[:, None, :], (decay.shape[0], DECAY_ROWS, decay.shape[1]))
    sent = jnp.concatenate([state, rows], axis=1).astype(jnp.bfloat16)
    everything = lax.all_gather(sent, axis)
    before = jnp.zeros_like(state)
    for k in range(count - 1):
        part = everything[k].astype(jnp.float32)
        new = part[:, depth : depth + 1] * before + part[:, :depth]
        before = jnp.where(k < index, new, before)
    return before


def mixer_half(
    recurrence_query_input,
    forget_gate_input,
    recurrence_value_input,
    output_gate_input,
    forget_lower_margin,
    position_decay_extra,
    head_norm_gain,
    recurrence_out_weight,
):
    length = recurrence_query_input.shape[0]
    head_tensor = position_decay_extra.shape[1]
    blocks = length // BLK
    queries = jax.nn.silu(recurrence_query_input.astype(jnp.float32))
    key_gate_value = forget_lower_margin[None, :] * jax.nn.sigmoid(
        -forget_gate_input.astype(jnp.float32)
    )
    decay_logarithm = jnp.log1p(-key_gate_value) + jnp.repeat(
        position_decay_extra, HEAD_CHANNELS, axis=1
    )
    value_rows = recurrence_value_input.astype(jnp.float32)

    def split_heads(tensor):
        return tensor.reshape(blocks, BLK, head_tensor, HEAD_CHANNELS).transpose(2, 0, 1, 3)

    query_heads = split_heads(queries)
    key_heads = split_heads(key_gate_value)
    value_heads = split_heads(value_rows)
    cum_decay = jnp.cumsum(split_heads(decay_logarithm), axis=2)
    middle = cum_decay[:, :, BLK // 2 - 1 : BLK // 2]
    block_end = cum_decay[:, :, BLK - 1 : BLK]
    scores = jnp.einsum(
        "hncd,hnsd->hncs",
        query_heads * jnp.exp(cum_decay - middle),
        key_heads * jnp.exp(middle - cum_decay),
        precision=PRECISION,
    )
    causal = jnp.tril(jnp.ones((BLK, BLK), dtype=bool))
    scores = jnp.where(causal, scores, 0.0)
    within = jnp.einsum("hncs,hnse->hnce", scores, value_heads, precision=PRECISION)
    updates = jnp.einsum(
        "hncd,hnce->nhed",
        key_heads * jnp.exp(block_end - cum_decay),
        value_heads,
        precision=PRECISION,
    )
    block_log = block_end[:, :, 0, :]
    block_decay = jnp.exp(block_log).transpose(1, 0, 2)

    state = jnp.zeros_like(updates[0])
    starts_list = []
    for block in range(blocks):
        starts_list.append(state)
        state = block_decay[block][:, None, :] * state + updates[block]
    local_final, local_starts = state, jnp.stack(starts_list)
    device_decay = jnp.exp(jnp.sum(block_log, axis=1))
    incoming = carried_in(device_decay, local_final, "ep")
    before = jnp.exp(jnp.cumsum(block_log, axis=1) - block_log).transpose(1, 0, 2)
    starts = local_starts + before[:, :, None, :] * incoming[None]
    carried = jnp.einsum(
        "hncd,nhed->hnce", query_heads * jnp.exp(cum_decay), starts, precision=PRECISION
    )
    outputs = (within + carried).transpose(1, 2, 0, 3).reshape(length, head_tensor, HEAD_CHANNELS)
    factor = lax.rsqrt(jnp.mean(outputs * outputs, axis=2, keepdims=True) + EPSILON)
    normed = (outputs * factor).reshape(length, head_tensor * HEAD_CHANNELS) * head_norm_gain[
        None, :
    ]
    gated_rows = (normed * jax.nn.silu(output_gate_input.astype(jnp.float32))).astype(jnp.bfloat16)
    partial = jnp.dot(
        gated_rows, recurrence_out_weight, preferred_element_type=jnp.float32
    ).astype(jnp.bfloat16)
    if lax.axis_size("tp") != 2:
        return lax.psum_scatter(partial, "tp", scatter_dimension=0, tiled=True)
    which, kept_rows = lax.axis_index("tp"), length // 2
    kept = lax.dynamic_slice_in_dim(partial, which * kept_rows, kept_rows)
    sent = lax.dynamic_slice_in_dim(partial, (1 - which) * kept_rows, kept_rows)
    received = lax.ppermute(sent, "tp", [(0, 1), (1, 0)])
    return (kept.astype(jnp.float32) + received.astype(jnp.float32)).astype(jnp.bfloat16)


def expert_half(
    expert_hidden_state,
    chosen_expert_index,
    chosen_expert_score,
    expert_norm_gain,
    routed_gate_weight,
    routed_up_weight,
    routed_down_weight,
    shared_gate_weight,
    shared_up_weight,
    shared_down_weight,
):
    tokens, top = chosen_expert_index.shape
    local_experts = routed_gate_weight.shape[0]
    devices = lax.axis_size("ep")
    experts = local_experts * devices
    capacity = min(tokens, 2 * tokens * top // experts)
    width_out = routed_down_weight.shape[2]
    features = expert_hidden_state.astype(jnp.float32)
    normed = (
        features
        * lax.rsqrt(jnp.mean(features * features, axis=1, keepdims=True) + EPSILON)
        * expert_norm_gain[None, :]
    ).astype(jnp.bfloat16)
    gates = ROUTED_SCALE * chosen_expert_score / jnp.sum(chosen_expert_score, axis=1, keepdims=True)
    flat_ids = chosen_expert_index.reshape(-1)
    onehot = (flat_ids[:, None] == jnp.arange(experts, dtype=jnp.int32)[None, :]).astype(jnp.int32)
    places = jnp.sum(onehot * (jnp.cumsum(onehot, axis=0) - 1), axis=1)
    slots = flat_ids * capacity + places
    owners = (
        jnp.full((experts * capacity,), tokens, jnp.int32)
        .at[slots]
        .set(jnp.arange(tokens * top, dtype=jnp.int32) // top)
    )
    padded = jnp.concatenate([normed, jnp.zeros((1, normed.shape[1]), jnp.bfloat16)], axis=0)
    outgoing = padded[owners].reshape(experts, capacity, normed.shape[1])
    piece = lax.all_to_all(outgoing, "ep", split_axis=0, concat_axis=0, tiled=True)
    grouped = piece.reshape(devices, local_experts, piece.shape[1], piece.shape[2])
    gate_part = jnp.einsum(
        "secd,edh->sech", grouped, routed_gate_weight, preferred_element_type=jnp.float32
    )
    up_part = jnp.einsum(
        "secd,edh->sech", grouped, routed_up_weight, preferred_element_type=jnp.float32
    )
    hidden = (jax.nn.silu(gate_part) * up_part).astype(jnp.bfloat16)
    hidden_rows = hidden.reshape(devices * local_experts, piece.shape[1], hidden.shape[3])
    flat_hidden = hidden_rows.reshape(experts * capacity, hidden_rows.shape[2])
    shared_hidden = (
        jax.nn.silu(jnp.dot(normed, shared_gate_weight, preferred_element_type=jnp.float32))
        * jnp.dot(normed, shared_up_weight, preferred_element_type=jnp.float32)
    ).astype(jnp.bfloat16)
    start_values = (
        jnp.zeros((experts * capacity, width_out), jnp.float32),
        jnp.zeros((tokens, width_out), jnp.float32),
    )
    routed_piece = lax.all_gather(flat_hidden, "tp", axis=1, tiled=True)
    shared_piece = lax.all_gather(shared_hidden, "tp", axis=1, tiled=True)
    count = routed_piece.shape[1]
    grouped = routed_piece.reshape(devices, local_experts, capacity, count)
    routed = jnp.einsum(
        "secn,enk->seck", grouped, routed_down_weight, preferred_element_type=jnp.float32
    )
    shared = jnp.dot(shared_piece, shared_down_weight, preferred_element_type=jnp.float32)
    routed_sum = routed.reshape(start_values[0].shape)
    answers = routed_sum.astype(jnp.bfloat16).reshape(experts, capacity, width_out)
    returned = lax.all_to_all(answers, "ep", split_axis=0, concat_axis=0, tiled=True)
    picked_rows = returned.reshape(experts * capacity, width_out)[slots].reshape(
        tokens, top, width_out
    )
    combined = shared + jnp.sum(gates[:, :, None] * picked_rows.astype(jnp.float32), axis=1)
    return combined.astype(jnp.bfloat16)


MESH = pl.DeviceIdType.MESH
LANES = 128


def expert_kernel(
    count,
    x_ref,
    gate_hbm,
    up_hbm,
    down_hbm,
    shared_gate_hbm,
    shared_up_hbm,
    shared_down_hbm,
    routed_ref,
    shared_ref,
    rows,
    gate_w,
    up_w,
    down_w,
    shared_gate_w,
    shared_up_w,
    shared_down_w,
    own_hidden,
    peer_hidden,
    load_sem,
    right_sem,
    left_sem,
    side_sem,
    row_sem,
    hidden_send,
    hidden_recv,
):
    chips = count // 2
    me = lax.axis_index("ep")
    half = lax.axis_index("tp")
    chip, core = me // 2, me % 2
    side = chip * 2 + 1 - core
    partner = 1 - half
    block_rows = x_ref.shape[0]
    width = gate_w.shape[0]
    units = gate_w.shape[1]
    has_right, has_left = chip < chips - 1, chip > 0

    def half_rows(ref, which):
        return ref.at[pl.ds(pl.multiple_of(which * units, units), units), :]

    loads = [
        (shared_gate_hbm, shared_gate_w),
        (shared_up_hbm, shared_up_w),
        (gate_hbm.at[0], gate_w),
        (up_hbm.at[0], up_w),
        (half_rows(down_hbm.at[0], half), down_w.at[0]),
        (half_rows(down_hbm.at[0], partner), down_w.at[1]),
        (half_rows(shared_down_hbm, half), shared_down_w.at[0]),
        (half_rows(shared_down_hbm, partner), shared_down_w.at[1]),
        (x_ref, rows.at[me]),
    ]
    copies = [
        pltpu.make_async_copy(source, target, load_sem.at[i])
        for i, (source, target) in enumerate(loads)
    ]
    for copy in copies:
        copy.start()

    barrier = pltpu.get_barrier_semaphore()
    pl.semaphore_signal(barrier, inc=1, device_id={"ep": side}, device_id_type=MESH)
    pl.semaphore_signal(barrier, inc=1, device_id={"tp": partner}, device_id_type=MESH)

    @pl.when(has_right)
    def _():
        pl.semaphore_signal(barrier, inc=1, device_id={"ep": me + 2}, device_id_type=MESH)

    @pl.when(has_left)
    def _():
        pl.semaphore_signal(barrier, inc=1, device_id={"ep": me - 2}, device_id_type=MESH)

    pl.semaphore_wait(barrier, 2 + has_right.astype(jnp.int32) + has_left.astype(jnp.int32))

    def row_copy(source, block, sems, target):
        return pltpu.make_async_remote_copy(
            src_ref=source,
            dst_ref=rows.at[block],
            send_sem=sems.at[block],
            recv_sem=row_sem.at[block],
            device_id={"ep": target},
            device_id_type=MESH,
        )

    def hidden_copy(step):
        return pltpu.make_async_remote_copy(
            src_ref=own_hidden.at[step],
            dst_ref=peer_hidden.at[step],
            send_sem=hidden_send.at[step],
            recv_sem=hidden_recv.at[step],
            device_id={"tp": partner},
            device_id_type=MESH,
        )

    def block_of(step):
        k, odd = step // 2, step % 2
        inner = jnp.minimum(chip, chips - 1 - chip)
        near = jnp.where(k % 2 == 1, chip - (k + 1) // 2, chip + k // 2)
        far = jnp.where(chip <= chips - 1 - chip, k, chips - 1 - k)
        source = jnp.where(k <= 2 * inner, near, far)
        return source, source * 2 + jnp.where(odd == 1, 1 - core, core)

    def goes_right(source):
        return jnp.logical_and(source <= chip, has_right)

    def goes_left(source):
        return jnp.logical_and(source >= chip, has_left)

    @pl.when(has_right)
    def _():
        row_copy(x_ref, me, right_sem, me + 2).start()

    @pl.when(has_left)
    def _():
        row_copy(x_ref, me, left_sem, me - 2).start()

    row_copy(x_ref, me, side_sem, side).start()

    copies[0].wait()
    copies[1].wait()
    gate_part = jnp.dot(
        x_ref[:, :width], shared_gate_w[...], preferred_element_type=jnp.float32
    )
    up_part = jnp.dot(x_ref[:, :width], shared_up_w[...], preferred_element_type=jnp.float32)
    own_hidden[count] = (jax.nn.silu(gate_part) * up_part).astype(jnp.bfloat16)
    for copy in copies[2:]:
        copy.wait()

    def down(step, weight):
        hidden_copy(step).wait_recv()
        return jnp.dot(
            own_hidden[step], weight[0], preferred_element_type=jnp.float32
        ) + jnp.dot(peer_hidden[step], weight[1], preferred_element_type=jnp.float32)

    def routed_down(step):
        _, block = block_of(step)
        place = pl.ds(pl.multiple_of(block * block_rows, block_rows), block_rows)
        routed_ref[place, :] = down(step, down_w).astype(jnp.bfloat16)

    def turn(step, _):
        source, block = block_of(step)
        odd = step % 2

        @pl.when(step > 0)
        def _():
            row_copy(x_ref, block, side_sem, side).wait_recv()

        @pl.when(jnp.logical_and(step > 0, odd == 0))
        def _():
            @pl.when(goes_right(source))
            def _():
                row_copy(rows.at[block], block, right_sem, me + 2).start()

            @pl.when(goes_left(source))
            def _():
                row_copy(rows.at[block], block, left_sem, me - 2).start()

            row_copy(rows.at[block], block, side_sem, side).start()

        x = rows[block, :, :width]
        tail = rows[block, :, width:].astype(jnp.float32)
        lane = lax.broadcasted_iota(jnp.int32, tail.shape, 1)
        own_gate = jnp.sum(
            jnp.where(lane % (LANES // 2) == me, tail, 0.0), axis=1, keepdims=True
        )
        gate_part = jnp.dot(x, gate_w[...], preferred_element_type=jnp.float32)
        up_part = jnp.dot(x, up_w[...], preferred_element_type=jnp.float32)
        own_hidden[step] = (jax.nn.silu(gate_part) * up_part * own_gate).astype(jnp.bfloat16)

        @pl.when(step == 0)
        def _():
            hidden_copy(count).start()

        @pl.when(step > 0)
        def _():
            routed_down(step - 1)

        hidden_copy(step).start()
        return 0

    lax.fori_loop(0, count, turn, 0)
    shared_ref[...] = down(count, shared_down_w)
    routed_down(count - 1)

    def finish(step, _):
        source, block = block_of(step)
        hidden_copy(step).wait_send()

        @pl.when(step % 2 == 0)
        def _():
            @pl.when(goes_right(source))
            def _():
                row_copy(x_ref, block, right_sem, me + 2).wait_send()

            @pl.when(goes_left(source))
            def _():
                row_copy(x_ref, block, left_sem, me - 2).wait_send()

            row_copy(x_ref, block, side_sem, side).wait_send()

        return 0

    lax.fori_loop(0, count, finish, 0)
    hidden_copy(count).wait_send()


def dense_expert_half(
    expert_hidden_state,
    chosen_expert_index,
    chosen_expert_score,
    expert_norm_gain,
    routed_gate_weight,
    routed_up_weight,
    routed_down_weight,
    shared_gate_weight,
    shared_up_weight,
    shared_down_weight,
):
    tokens = chosen_expert_index.shape[0]
    count = lax.axis_size("ep")
    features = expert_hidden_state.astype(jnp.float32)
    width = features.shape[1]
    units, width_out = routed_gate_weight.shape[2], routed_down_weight.shape[2]
    normed = (
        features
        * lax.rsqrt(jnp.mean(features * features, axis=1, keepdims=True) + EPSILON)
        * expert_norm_gain[None, :]
    ).astype(jnp.bfloat16)
    gates = ROUTED_SCALE * chosen_expert_score / jnp.sum(chosen_expert_score, axis=1, keepdims=True)
    slots = LANES // 2
    chosen = chosen_expert_index[:, :, None] == jnp.arange(slots, dtype=jnp.int32)[None, None, :]
    gate_table = jnp.sum(jnp.where(chosen, gates[:, :, None], 0.0), axis=1)
    high = gate_table.astype(jnp.bfloat16)
    low = (gate_table - high.astype(jnp.float32)).astype(jnp.bfloat16)
    sent = jnp.concatenate([normed, high, low], axis=1)
    hbm = pl.BlockSpec(memory_space=pl.ANY)
    vmem = pl.BlockSpec(memory_space=pltpu.VMEM)
    weight = pltpu.VMEM((width, units), jnp.bfloat16)
    down_weight = pltpu.VMEM((2, units, width_out), jnp.bfloat16)
    hidden = pltpu.VMEM((count + 1, tokens, units), jnp.bfloat16)
    block_sems = pltpu.SemaphoreType.DMA((count,))
    routed, shared = pl.pallas_call(
        functools.partial(expert_kernel, count),
        out_shape=(
            jax.ShapeDtypeStruct((count * tokens, width_out), jnp.bfloat16),
            jax.ShapeDtypeStruct((tokens, width_out), jnp.float32),
        ),
        in_specs=[vmem] + [hbm] * 6,
        out_specs=(vmem, vmem),
        scratch_shapes=[
            pltpu.VMEM((count, tokens, width + LANES), jnp.bfloat16),
            weight,
            weight,
            down_weight,
            weight,
            weight,
            down_weight,
            hidden,
            hidden,
            pltpu.SemaphoreType.DMA((9,)),
            block_sems,
            block_sems,
            block_sems,
            block_sems,
            pltpu.SemaphoreType.DMA((count + 1,)),
            pltpu.SemaphoreType.DMA((count + 1,)),
        ],
        compiler_params=pltpu.CompilerParams(
            collective_id=0, has_side_effects=True, vmem_limit_bytes=48 * 1024 * 1024
        ),
        cost_estimate=pl.CostEstimate(
            flops=45_000_000_000, bytes_accessed=16_000_000, transcendentals=0
        ),
        name="expert_kernel",
    )(
        sent,
        routed_gate_weight,
        routed_up_weight,
        routed_down_weight,
        shared_gate_weight,
        shared_up_weight,
        shared_down_weight,
    )
    total = lax.psum_scatter(routed, "ep", scatter_dimension=0, tiled=True)
    return (shared + total.astype(jnp.float32)).astype(jnp.bfloat16)


def per_device(
    recurrence_query_input,
    forget_gate_input,
    recurrence_value_input,
    output_gate_input,
    forget_lower_margin,
    position_decay_extra,
    head_norm_gain,
    recurrence_out_weight,
    expert_hidden_state,
    chosen_expert_index,
    chosen_expert_score,
    expert_norm_gain,
    routed_gate_weight,
    routed_up_weight,
    routed_down_weight,
    shared_gate_weight,
    shared_up_weight,
    shared_down_weight,
):
    recurrence_output = mixer_half(
        recurrence_query_input,
        forget_gate_input,
        recurrence_value_input,
        output_gate_input,
        forget_lower_margin,
        position_decay_extra,
        head_norm_gain,
        recurrence_out_weight,
    )
    tokens, top = chosen_expert_index.shape
    experts = routed_gate_weight.shape[0] * lax.axis_size("ep")
    every_row_fits = 2 * top >= experts and routed_gate_weight.shape[0] == 1 and experts <= 64
    half = dense_expert_half if every_row_fits else expert_half
    expert_out = half(
        expert_hidden_state,
        chosen_expert_index,
        chosen_expert_score,
        expert_norm_gain,
        routed_gate_weight,
        routed_up_weight,
        routed_down_weight,
        shared_gate_weight,
        shared_up_weight,
        shared_down_weight,
    )
    return (recurrence_output, expert_out)


def solution(mesh):
    in_specs = (
        P(("grp", "ep"), "tp"),
        P(("grp", "ep"), "tp"),
        P(("grp", "ep"), "tp"),
        P(("grp", "ep"), "tp"),
        P("tp"),
        P(("grp", "ep"), "tp"),
        P("tp"),
        P("tp", None),
        P(("grp", "ep"), None),
        P(("grp", "ep"), None),
        P(("grp", "ep"), None),
        P(),
        P("ep", None, "tp"),
        P("ep", None, "tp"),
        P("ep", None, "tp"),
        P(None, "tp"),
        P(None, "tp"),
        P(None, "tp"),
    )
    out_specs = (P(("grp", "ep", "tp"), None), P(("grp", "ep"), "tp"))
    return jax.shard_map(
        per_device, mesh=mesh, in_specs=in_specs, out_specs=out_specs, check_vma=False
    )
```
